32 devices in a mesh: fs: 4 (over y, x), tp: 8 (over z, core).
Axes of the slice: x: 2, y: 2, z: 4, core: 2. Of those that a mesh axis runs over, the one named last changes fastest.
Arguments:
- tokens: bfloat16 [1024, 2048], P('fs', 'tp'), may hold values from -60 to 60
- norm_gain: float32 [2048], P('fs'), may hold values from 0.1 to 1.9
- gate_weight: float32 [4, 2048, 4096], P(None, 'fs', 'tp'), may hold values from -0.125 to 0.125
- up_weight: float32 [4, 2048, 4096], P(None, 'fs', 'tp'), may hold values from -0.125 to 0.125
- down_weight: float32 [4, 2048, 4096], P(None, 'fs', 'tp'), may hold values from -0.125 to 0.125
- route: int32 [1024, 2], P('fs'), may hold values from 0 to 3, all different within a row; in each aligned block of 256 rows (0 to 255, 256 to 511, ...) at most 256 rows name the same one
- route_weight: float32 [1024, 2], P('fs'), may hold values from 0.2 to 1
Outputs:
- mixed: bfloat16 [1024, 2048], P('fs', 'tp')
- gate_new: bfloat16 [4, 2048, 4096], P('fs', None, 'tp')
- up_new: bfloat16 [4, 2048, 4096], P('fs', None, 'tp')
- down_new: bfloat16 [4, 2048, 4096], P('fs', None, 'tp')
The draws below stay inside these ranges and needn't reach their ends.
Inputs may be any that keep to these rules, and one draw needn't show every extreme that they name: `route`: the 2 experts of a row differ. In each aligned block of 256 rows (the tokens of one index of fs) no expert is named by more than 256 rows, a bound that some block reaches.
All inputs are finite; a program needn't handle non-finite values.
Results may differ from the reference program's by a relative error of at most 0.024.
Values may be sent and summed in bfloat16 or wider, within the bound.
No kernel may reach another device: no remote copies, remote signals or barrier semaphores. Data moves between devices by JAX's collectives and lax.ppermute only.
A program may use at most 64 MiB of HBM per device.

```python
import math
import jax
import jax.numpy as jnp
import numpy as np
from jax import lax

D = 2048
FF = 4096
TOP = 2
TOK_DEV = 256
EXPERTS = 4
CAP = 256
TOKENS = 1024
N_FS = 4
N_TP = 8


def draw_tokens(key, part):
    key_base = jax.random.fold_in(key, 11)
    values = jax.random.normal(key_base, (TOKENS, D), jnp.float32)
    column_scale = 0.6 * 3.0 ** (jnp.arange(D, dtype=jnp.float32) / D)
    values = jnp.clip(values * column_scale[None, :], -60.0, 60.0)
    return values.astype(jnp.bfloat16)


def strengthened(result, own_key, source, target, parts, factor):
    def block_of(dim):
        return (jnp.arange(result.shape[dim]) // (result.shape[dim] // parts)).reshape((-1,) + (1,) * (result.ndim - 1 - dim))

    first = jax.random.permutation(own_key, parts)[block_of(target)]
    other_side = (block_of(target) + parts // 2) % parts
    return jnp.where((block_of(source) == first) | (block_of(source) == other_side), factor * result, result)


def block_levels(rng, extent, cuts, least, top_value):
    gain = 1.0
    for dim, blocks in cuts:
        heights = jax.random.uniform(jax.random.fold_in(jax.random.fold_in(rng, 6), dim), (blocks,), jnp.float32, least / len(cuts), top_value / len(cuts))
        gain = gain * jnp.repeat(jnp.exp(heights), extent[dim] // blocks).reshape((-1,) + (1,) * (len(extent) - 1 - dim))
    return gain


def assign_block(stream_key, own, number, rows, amount, top, bound, slope):
    ranking = jax.random.permutation(stream_key, amount)
    heavy_load, ordinary = portions_of(amount, rows * top, bound, slope, True), portions_of(amount, rows * top, bound, slope, False)
    places = jnp.arange(amount)

    def named(tallies, offset_by):
        used = int((tallies > 0).sum())
        fixed = max(1, used // 4)
        moved = fixed + (places - fixed + offset_by * (used - fixed)) % max(1, amount - fixed)
        return jnp.zeros((amount,), jnp.int32).at[ranking[jnp.where(places < fixed, places, moved)]].set(jnp.asarray(tallies, jnp.int32))

    tallies = jnp.where(number % 4 == 0, named(heavy_load, number // 4), named(ordinary, number - number // 4 - 1))
    mixed = jax.random.permutation(jax.random.fold_in(own, 3), amount)
    donor, receiver = mixed[0:amount // 2 * 2:2], mixed[1:amount // 2 * 2:2]
    slack = jnp.minimum(tallies[donor] - 1, bound - tallies[receiver]) // 2
    slack = jnp.where((donor == ranking[0]) | (receiver == ranking[0]) | (tallies[receiver] == 0), 0, jnp.maximum(slack, 0))
    moved = jax.random.randint(jax.random.fold_in(own, 4), (amount // 2,), 0, 1 << 20) % (slack + 1)
    tallies = tallies.at[donor].add(-moved).at[receiver].add(moved)
    members = jnp.searchsorted(jnp.cumsum(tallies), jnp.arange(rows * top), side="right").astype(jnp.int32)
    table = members.reshape(top, rows).T
    table = table[jax.random.permutation(jax.random.fold_in(own, 1), rows)]
    offset_by = jax.random.randint(jax.random.fold_in(own, 2), (rows, 1), 0, top)
    return jnp.take_along_axis(table, (jnp.arange(top)[None, :] + offset_by) % top, axis=1)


def portions_of(amount, total, reach, skew, full):
    weights = [(1 << 20) // math.isqrt(grade ** skew) + 1 for grade in range(1, amount + 1)]
    largest = reach if full else min(reach, max(-(-total // amount), total * weights[0] // sum(weights)))
    least = 1 if total - largest >= amount - 1 else 0
    given, spare = [largest] + [least] * (amount - 1), total - largest - least * (amount - 1)
    while spare > 0:
        candidates = [i for i in range(1, amount) if given[i] < largest] or [i for i in range(1, amount) if given[i] < reach]
        pool, remaining = sum([weights[i] for i in candidates]), spare
        for i in candidates:
            more = min(reach - given[i], max(1, remaining * weights[i] // pool), spare)
            given[i] = given[i] + more
            spare = spare - more
    return np.array(given)


def noise(rng, dims, spread, bound, pieces=(), kind=jnp.bfloat16):
    factor_of = block_levels(rng, dims, pieces, -0.22, 0.18) if pieces else 1.0
    entries = jax.random.normal(rng, dims, jnp.float32) * spread * factor_of
    return jnp.minimum(jnp.maximum(entries, -bound), bound).astype(kind)


def gaussian_with(stream_key, extent, spread, most, split, heavy, kind=jnp.bfloat16):
    drawn = spread * jax.random.normal(stream_key, extent, jnp.float32)
    if split:
        drawn = drawn * block_levels(stream_key, extent, split, -0.22, 0.18)
    return jnp.clip(strengthened(drawn, jax.random.fold_in(stream_key, 3), *heavy), -most, most).astype(kind)


def setup_inputs(seed: int = 0) -> dict:
    streams_of = jax.random.split(jax.random.key(seed), 8)
    tokens = draw_tokens(jax.random.fold_in(streams_of[7], 71), 0)
    norm_gain = jnp.clip(1.0 + 0.18 * jax.random.normal(streams_of[1], (D,), jnp.float32), 0.1, 1.9)
    gate_weight = noise(streams_of[2], (EXPERTS, D, FF), D ** -0.5, 0.125, ((1, 4), (2, 8)), jnp.float32)
    up_weight = noise(streams_of[3], (EXPERTS, D, FF), D ** -0.5, 0.125, ((1, 4), (2, 8)), jnp.float32)
    down_weight = gaussian_with(streams_of[4], (EXPERTS, D, FF), FF ** -0.5, 0.125, ((1, 4), (2, 8)), (2, 1, 8, 2.0), jnp.float32)
    route_keys = jax.random.split(jax.random.fold_in(streams_of[5], 1), TOKENS // TOK_DEV)
    route_turns = jax.random.permutation(jax.random.fold_in(streams_of[5], 3), TOKENS // TOK_DEV)
    route = jax.vmap(lambda own, number: assign_block(jax.random.fold_in(streams_of[5], 2), own, number, TOK_DEV, EXPERTS, TOP, CAP, 2))(route_keys, route_turns).reshape((TOKENS, TOP))
    route_weight = jnp.clip(jnp.exp(math.log(1.0) - 1.609438 * jax.random.uniform(streams_of[6], (TOKENS, TOP), jnp.float32) ** block_levels(streams_of[6], (TOKENS, TOP), ((0, 4),), -0.2, 0.2)), 0.2, 1.0)
    return {"tokens": tokens, "norm_gain": norm_gain, "gate_weight": gate_weight, "up_weight": up_weight, "down_weight": down_weight, "route": route, "route_weight": route_weight}


epsilon = 1e-05

def slot_table(route, block_rows, expert_count):
    pair_ids = route.reshape(-1, block_rows * route.shape[1])
    onehot = (pair_ids[:, :, None] == jnp.arange(expert_count, dtype=jnp.int32)[None, None, :]).astype(jnp.int32)
    before = jnp.cumsum(onehot, axis=1) - onehot
    return lax.optimization_barrier(jnp.sum(before * onehot, axis=2)).astype(jnp.int32).reshape(route.shape)

def reference(tokens, norm_gain, gate_weight, up_weight, down_weight, route, route_weight):
    gain_col = norm_gain.astype(jnp.float32)[None, :, None]
    gate_new = (gate_weight * gain_col).astype(jnp.bfloat16)
    up_new = (up_weight * gain_col).astype(jnp.bfloat16)
    down_new = down_weight.astype(jnp.bfloat16)
    tok_float = tokens.astype(jnp.float32)
    normed = (tok_float * lax.rsqrt(lax.optimization_barrier(jnp.mean(tok_float * tok_float, axis=1, keepdims=True)) + epsilon)).astype(jnp.bfloat16)
    slot_of = slot_table(route, TOK_DEV, EXPERTS)
    groups = jnp.broadcast_to((jnp.arange(TOKENS, dtype=jnp.int32) // TOK_DEV)[:, None], route.shape)
    token_index = jnp.broadcast_to(jnp.arange(TOKENS, dtype=jnp.int32)[:, None], route.shape)
    row_table = jnp.full((EXPERTS, N_FS, CAP), TOKENS, jnp.int32).at[route, groups, slot_of].set(token_index)
    padded = jnp.concatenate([normed, jnp.zeros((1, D), jnp.bfloat16)], axis=0)
    block_width = FF // N_TP

    def one_expert(operands):
        gate_e, up_e, down_e, rows_e = operands
        expert_rows = padded[rows_e.reshape(-1)]
        gate_acc = jnp.dot(expert_rows, gate_e, preferred_element_type=jnp.float32)
        up_acc = jnp.dot(expert_rows, up_e, preferred_element_type=jnp.float32)
        hidden = (jax.nn.silu(gate_acc) * up_acc).astype(jnp.bfloat16)

        def add_block(block, running):
            offset = jnp.asarray(block, jnp.int32) * block_width
            part_hidden = lax.dynamic_slice_in_dim(hidden, offset, block_width, 1)
            part_weight = lax.dynamic_slice_in_dim(down_e, offset, block_width, 1)
            term = lax.dot_general(part_hidden, part_weight, (((1,), (1,)), ((), ())), preferred_element_type=jnp.float32)
            return running + term.astype(jnp.bfloat16).astype(jnp.float32)
        summed = lax.fori_loop(0, N_TP, add_block, jnp.zeros((N_FS * CAP, D), jnp.float32))
        return summed.astype(jnp.bfloat16)
    outputs = lax.map(one_expert, (gate_new, up_new, down_new, row_table))
    flat = outputs.reshape(EXPERTS * N_FS * CAP, D)
    index = ((route * N_FS + groups) * CAP + slot_of).astype(jnp.int32)
    picked = flat[index].astype(jnp.float32)
    mixed = lax.optimization_barrier(jnp.sum(picked * route_weight.astype(jnp.float32)[:, :, None], axis=1)).astype(jnp.bfloat16)
    return (mixed, gate_new, up_new, down_new)
```

```python
import jax
import jax.numpy as jnp
from jax import lax
from jax.sharding import PartitionSpec as P

epsilon = 1e-05


def slot_table(route, block_rows, expert_count):
    pair_ids = route.reshape(-1, block_rows * route.shape[1])
    onehot = (
        pair_ids[:, :, None] == jnp.arange(expert_count, dtype=jnp.int32)[None, None, :]
    ).astype(jnp.int32)
    before = jnp.cumsum(onehot, axis=1) - onehot
    return jnp.sum(before * onehot, axis=2).reshape(route.shape)


def sparse_body(tokens, norm_gain, gate_weight, up_weight, down_weight, route, route_weight):
    experts = gate_weight.shape[0]
    tok_rows = tokens.shape[0]
    columns = tokens.shape[1]
    fs_count = lax.axis_size("fs")
    capacity = 4 * tok_rows // fs_count
    gain_col = norm_gain[None, :, None]
    gate_cast = (gate_weight * gain_col).astype(jnp.bfloat16)
    up_cast = (up_weight * gain_col).astype(jnp.bfloat16)
    down_cast = down_weight.astype(jnp.bfloat16)
    gate_new, up_new, down_new = (
        lax.all_to_all(gate_cast, "fs", split_axis=0, concat_axis=1, tiled=True),
        lax.all_to_all(up_cast, "fs", split_axis=0, concat_axis=1, tiled=True),
        lax.all_to_all(down_cast, "fs", split_axis=0, concat_axis=1, tiled=True),
    )
    slot_of = slot_table(route, tok_rows, experts)
    target = route * capacity + slot_of
    slot_lanes = jnp.arange(experts * capacity, dtype=jnp.int32)
    slot_hits = target[:, :, None] == slot_lanes[None, None, :]
    token_iota = jnp.arange(tok_rows, dtype=jnp.int32)[:, None, None]
    lane_token = jnp.sum(jnp.where(slot_hits, token_iota + 1, 0), axis=(0, 1)) - 1
    lane_token = jnp.where(lane_token < 0, tok_rows, lane_token)
    combine = jnp.sum(jnp.where(slot_hits, route_weight[:, :, None], 0.0), axis=1)
    tok_float = tokens.astype(jnp.float32)
    square_sum = lax.psum(jnp.sum(tok_float * tok_float, axis=1), "tp")
    full_width = columns * lax.axis_size("tp")
    normed = (tok_float * lax.rsqrt(square_sum / full_width + epsilon)[:, None]).astype(
        jnp.bfloat16
    )
    padded = jnp.concatenate([normed, jnp.zeros((1, columns), jnp.bfloat16)], axis=0)
    outgoing = padded[lane_token].reshape(experts, capacity, columns)
    arrived = lax.all_to_all(outgoing, "fs", split_axis=0, concat_axis=0, tiled=True).reshape(
        -1, columns
    )
    piece_rows = lax.all_gather(arrived, "tp", axis=1, tiled=True)
    gate_acc = jnp.dot(piece_rows, gate_new[0], preferred_element_type=jnp.float32)
    up_acc = jnp.dot(piece_rows, up_new[0], preferred_element_type=jnp.float32)
    hidden = (jax.nn.silu(gate_acc) * up_acc).astype(jnp.bfloat16)
    summed = lax.psum_scatter(
        lax.dot_general(
            down_new[0], hidden, (((1,), (1,)), ((), ())), preferred_element_type=jnp.float32
        ).astype(jnp.bfloat16),
        "tp",
        scatter_dimension=0,
        tiled=True,
    )
    own_columns = summed.shape[0]
    outgoing_back = summed.reshape(own_columns, fs_count, capacity)
    returned = lax.all_to_all(outgoing_back, "fs", split_axis=1, concat_axis=1, tiled=True).reshape(
        own_columns, experts * capacity
    )
    mixed = lax.dot_general(
        combine,
        returned.astype(jnp.float32),
        (((1,), (1,)), ((), ())),
        precision=lax.Precision.HIGHEST,
        preferred_element_type=jnp.float32,
    )
    return (mixed.astype(jnp.bfloat16), gate_new, up_new, down_new)


def swap(x, axis, distance):
    count = lax.axis_size(axis)
    return lax.ppermute(x, axis, [(s, s ^ distance) for s in range(count)])


def after(x, *others):
    return lax.optimization_barrier((x,) + others)[0]


def dense_body(tokens, norm_gain, gate_weight, up_weight, down_weight, route, route_weight):
    bf16, f32 = jnp.bfloat16, jnp.float32
    fs_count, tp_count = lax.axis_size("fs"), lax.axis_size("tp")
    z_count = tp_count // 2
    fs_id, tp_id = lax.axis_index("fs"), lax.axis_index("tp")
    z_id, core = tp_id // 2, tp_id % 2
    tok_rows, columns = tokens.shape
    width = columns * tp_count
    part_rows, hidden_cols = gate_weight.shape[1], gate_weight.shape[2]
    gain_col = norm_gain[:, None]
    halves = 2
    piece = columns // halves

    def expert_of(weight, k):
        return lax.dynamic_index_in_dim(weight, fs_id ^ k, 0, keepdims=False)

    order = sorted(range(1, fs_count), key=lambda k: (-bin(k).count("1"), k))
    fs_tokens = {k: swap(tokens, "fs", k) for k in order}
    fs_tokens[0] = tokens

    def exchange(pieces):
        got = {k: swap(pieces[k], "fs", k) for k in order}
        got[0] = pieces[0]
        return got

    gate_got = exchange(
        {k: (expert_of(gate_weight, k) * gain_col).astype(bf16) for k in range(fs_count)}
    )
    up_got = exchange(
        {k: (expert_of(up_weight, k) * gain_col).astype(bf16) for k in range(fs_count)}
    )
    down_parts = {
        k: expert_of(down_weight, k).astype(bf16).reshape(2, halves, piece, hidden_cols)
        for k in range(fs_count)
    }
    down_got = [exchange({k: v[:, h] for k, v in down_parts.items()}) for h in range(halves)]

    block = jnp.concatenate([fs_tokens[k] for k in range(fs_count)], axis=0)
    own_side = {m: swap(block, "tp", 2 * m) for m in range(1, z_count)}
    own_side[0] = block
    other_side = {m: swap(own_side[m], "tp", 1) for m in range(z_count)}

    def assemble(got):
        full = jnp.zeros((fs_count,) + got[0].shape, bf16)
        for k in range(fs_count):
            full = lax.dynamic_update_index_in_dim(full, got[k], fs_id ^ k, 0)
        return full

    gate_full, up_full = assemble(gate_got), assemble(up_got)
    square_sum = sum(
        jnp.sum(jnp.square(v.astype(f32)), axis=1)
        for v in list(own_side.values()) + list(other_side.values())
    )
    row_scale = lax.rsqrt(square_sum / width + epsilon)[:, None]

    def product(full):
        blocks = full.reshape(tp_count, columns, hidden_cols)
        total = 0.0
        for m in range(z_count):
            for side, which in ((own_side, core), (other_side, 1 - core)):
                weight = lax.dynamic_index_in_dim(
                    blocks, 2 * (z_id ^ m) + which, 0, keepdims=False
                )
                total = total + jnp.dot(side[m], weight, preferred_element_type=f32)
        return total

    gate_acc = product(gate_full) * row_scale
    up_acc = product(up_full) * row_scale
    hidden = (jax.nn.silu(gate_acc) * up_acc).astype(bf16)

    expert_ids = route[:, :, None] == (fs_id ^ jnp.arange(fs_count, dtype=jnp.int32))[None, None, :]
    share = jnp.sum(jnp.where(expert_ids, route_weight[:, :, None], 0.0), axis=1)

    down_halves, mixed = [], []
    for h in range(halves):
        full = assemble(down_got[h])
        down_halves.append(full)

        def partial(which):
            rows = [
                lax.dynamic_index_in_dim(
                    lax.dynamic_index_in_dim(full, z_id ^ m, 0, keepdims=False),
                    which,
                    0,
                    keepdims=False,
                )
                for m in range(z_count)
            ]
            return lax.dot_general(
                hidden,
                jnp.concatenate(rows, axis=0),
                (((1,), (1,)), ((), ())),
                preferred_element_type=f32,
            )

        came = swap(partial(1 - core).astype(bf16), "tp", 1)
        total = (partial(core) + came.astype(f32)).astype(bf16)
        slots = [total[:, m * piece : (m + 1) * piece] for m in range(z_count)]
        step = 1
        while step < z_count:
            sent = jnp.concatenate(slots[1::2], axis=1)
            kept = jnp.concatenate(slots[0::2], axis=1)
            came = swap(sent, "tp", 2 * step)
            total = (kept.astype(f32) + came.astype(f32)).astype(bf16)
            slots = [total[:, m * piece : (m + 1) * piece] for m in range(len(slots) // 2)]
            step *= 2
        outs = [slots[0][k * tok_rows : (k + 1) * tok_rows] for k in range(fs_count)]
        back = exchange(dict(enumerate(outs)))
        mixed.append(
            sum(share[:, k : k + 1] * back[k].astype(f32) for k in range(fs_count)).astype(bf16)
        )

    down_full = jnp.stack(down_halves, axis=2)
    shape = (1, fs_count * part_rows, hidden_cols)
    return (
        jnp.concatenate(mixed, axis=1),
        gate_full.reshape(shape),
        up_full.reshape(shape),
        down_full.reshape(shape),
    )


def body(tokens, norm_gain, gate_weight, up_weight, down_weight, route, route_weight):
    fs_count, tp_count = lax.axis_size("fs"), lax.axis_size("tp")
    power = fs_count & (fs_count - 1) == 0
    dense = power and 2 * fs_count == tp_count and fs_count == gate_weight.shape[0] and fs_count <= 4
    run = dense_body if dense else sparse_body
    return run(tokens, norm_gain, gate_weight, up_weight, down_weight, route, route_weight)


def solution(mesh):
    in_specs = (
        P("fs", "tp"),
        P("fs"),
        P(None, "fs", "tp"),
        P(None, "fs", "tp"),
        P(None, "fs", "tp"),
        P("fs", None),
        P("fs", None),
    )
    out_specs = (P("fs", "tp"), P("fs", None, "tp"), P("fs", None, "tp"), P("fs", None, "tp"))
    return jax.shard_map(body, mesh=mesh, in_specs=in_specs, out_specs=out_specs, check_vma=False)
```

```python
import jax
import jax.numpy as jnp
from jax import lax
from jax.experimental import pallas as pl
from jax.experimental.pallas import tpu as pltpu
from jax.sharding import PartitionSpec as P

epsilon = 1e-05


def slot_table(route, block_rows, expert_count):
    pair_ids = route.reshape(-1, block_rows * route.shape[1])
    onehot = (
        pair_ids[:, :, None] == jnp.arange(expert_count, dtype=jnp.int32)[None, None, :]
    ).astype(jnp.int32)
    before = jnp.cumsum(onehot, axis=1) - onehot
    return jnp.sum(before * onehot, axis=2).reshape(route.shape)


def sparse_body(tokens, norm_gain, gate_weight, up_weight, down_weight, route, route_weight):
    experts = gate_weight.shape[0]
    tok_rows = tokens.shape[0]
    columns = tokens.shape[1]
    fs_count = lax.axis_size("fs")
    capacity = 4 * tok_rows // fs_count
    gain_col = norm_gain[None, :, None]
    gate_cast = (gate_weight * gain_col).astype(jnp.bfloat16)
    up_cast = (up_weight * gain_col).astype(jnp.bfloat16)
    down_cast = down_weight.astype(jnp.bfloat16)
    gate_new, up_new, down_new = (
        lax.all_to_all(gate_cast, "fs", split_axis=0, concat_axis=1, tiled=True),
        lax.all_to_all(up_cast, "fs", split_axis=0, concat_axis=1, tiled=True),
        lax.all_to_all(down_cast, "fs", split_axis=0, concat_axis=1, tiled=True),
    )
    slot_of = slot_table(route, tok_rows, experts)
    target = route * capacity + slot_of
    slot_lanes = jnp.arange(experts * capacity, dtype=jnp.int32)
    slot_hits = target[:, :, None] == slot_lanes[None, None, :]
    token_iota = jnp.arange(tok_rows, dtype=jnp.int32)[:, None, None]
    lane_token = jnp.sum(jnp.where(slot_hits, token_iota + 1, 0), axis=(0, 1)) - 1
    lane_token = jnp.where(lane_token < 0, tok_rows, lane_token)
    combine = jnp.sum(jnp.where(slot_hits, route_weight[:, :, None], 0.0), axis=1)
    tok_float = tokens.astype(jnp.float32)
    square_sum = lax.psum(jnp.sum(tok_float * tok_float, axis=1), "tp")
    full_width = columns * lax.axis_size("tp")
    normed = (tok_float * lax.rsqrt(square_sum / full_width + epsilon)[:, None]).astype(
        jnp.bfloat16
    )
    padded = jnp.concatenate([normed, jnp.zeros((1, columns), jnp.bfloat16)], axis=0)
    outgoing = padded[lane_token].reshape(experts, capacity, columns)
    arrived = lax.all_to_all(outgoing, "fs", split_axis=0, concat_axis=0, tiled=True).reshape(
        -1, columns
    )
    piece_rows = lax.all_gather(arrived, "tp", axis=1, tiled=True)
    gate_acc = jnp.dot(piece_rows, gate_new[0], preferred_element_type=jnp.float32)
    up_acc = jnp.dot(piece_rows, up_new[0], preferred_element_type=jnp.float32)
    hidden = (jax.nn.silu(gate_acc) * up_acc).astype(jnp.bfloat16)
    summed = lax.psum_scatter(
        lax.dot_general(
            down_new[0], hidden, (((1,), (1,)), ((), ())), preferred_element_type=jnp.float32
        ).astype(jnp.bfloat16),
        "tp",
        scatter_dimension=0,
        tiled=True,
    )
    own_columns = summed.shape[0]
    outgoing_back = summed.reshape(own_columns, fs_count, capacity)
    returned = lax.all_to_all(outgoing_back, "fs", split_axis=1, concat_axis=1, tiled=True).reshape(
        own_columns, experts * capacity
    )
    mixed = lax.dot_general(
        combine,
        returned.astype(jnp.float32),
        (((1,), (1,)), ((), ())),
        precision=lax.Precision.HIGHEST,
        preferred_element_type=jnp.float32,
    )
    return (mixed.astype(jnp.bfloat16), gate_new, up_new, down_new)


def far_last(count):
    powers = [m for m in range(1, count) if m & (m - 1) == 0]
    return powers[::-1] + [m for m in range(1, count) if m & (m - 1)]


def far_first(count):
    return sorted(range(1, count), key=lambda k: (-bin(k).count("1"), k))


def swap(x, axis, distance):
    count = lax.axis_size(axis)
    return lax.ppermute(x, axis, [(s, s ^ distance) for s in range(count)])


def local_kernel(body, outs, flops=0, moved=0, extra=0, **kwargs):
    def call(*operands):
        held = sum(x.size * x.dtype.itemsize for x in operands)
        held += sum(x.size * x.dtype.itemsize for x in jax.tree.leaves(outs))
        return pl.pallas_call(
            body,
            out_shape=outs,
            cost_estimate=pl.CostEstimate(flops=flops, bytes_accessed=moved, transcendentals=0),
            compiler_params=pltpu.CompilerParams(vmem_limit_bytes=held + extra + GRANT),
            **kwargs,
        )(*operands)

    return call


GRANT = 4 << 20
HBM = pl.BlockSpec(memory_space=pltpu.HBM)
SMEM = pl.BlockSpec(memory_space=pltpu.SMEM)
VMEM = pl.BlockSpec(memory_space=pltpu.VMEM)


def cast_scaled(ids, weight, gain):
    count, rows, cols = weight.shape
    tile = 128

    def kernel(ids_ref, w_ref, gain_ref, *out_refs):
        for r in range(0, rows, tile):
            column = jnp.broadcast_to(gain_ref[:, r : r + tile], (tile, tile)).T
            column = jnp.concatenate([column] * (cols // tile), axis=1)
            for k in range(count):
                scaled = w_ref[ids_ref[0] ^ k, r : r + tile] * column
                out_refs[k][r : r + tile, :] = scaled.astype(jnp.bfloat16)

    return local_kernel(
        kernel,
        [jax.ShapeDtypeStruct((rows, cols), jnp.bfloat16)] * count,
        2 * weight.size,
        6 * weight.size,
        in_specs=[SMEM, VMEM, VMEM],
        out_specs=[VMEM] * count,
    )(ids, weight, gain[None, :])


def cast_pieces(ids, weight, pieces):
    count, rows, cols = weight.shape
    piece = rows // 2 // pieces

    def kernel(ids_ref, w_ref, *out_refs):
        for h in range(pieces):
            for k in range(count):
                for side in range(2):
                    start = side * (rows // 2) + h * piece
                    out_refs[h * count + k][side] = w_ref[
                        ids_ref[0] ^ k, start : start + piece
                    ].astype(jnp.bfloat16)

    outs = local_kernel(
        kernel,
        [jax.ShapeDtypeStruct((2, piece, cols), jnp.bfloat16)] * (count * pieces),
        2 * weight.size,
        6 * weight.size,
        in_specs=[SMEM, VMEM],
        out_specs=[VMEM] * (count * pieces),
    )(ids, weight)
    return [list(outs[h * count : (h + 1) * count]) for h in range(pieces)]


def stack_rows(parts):
    rows, cols = parts[0].shape

    def kernel(*refs):
        for k in range(len(parts)):
            refs[-1][k * rows : (k + 1) * rows, :] = refs[k][...]

    return local_kernel(
        kernel,
        jax.ShapeDtypeStruct((len(parts) * rows, cols), parts[0].dtype),
        0,
        4 * len(parts) * rows * cols,
        in_specs=[VMEM] * len(parts),
        out_specs=VMEM,
    )(*parts)


def lay_rows(ids_ref, part_refs, full_ref, w_ref, sems, columns):
    part_rows = part_refs[0].shape[0]
    copies = []
    for k, ref in enumerate(part_refs):
        at = pl.multiple_of((ids_ref[0] ^ k) * part_rows, part_rows)
        copies.append(pltpu.make_async_copy(ref, full_ref.at[pl.ds(at, part_rows)], sems.at[k]))
        copies[-1].start()
    for k, ref in enumerate(part_refs):
        m = ids_ref[0] ^ ids_ref[1] ^ k
        for s in range(2):
            to = pl.multiple_of((2 * m + s) * columns, columns)
            at = pl.multiple_of((ids_ref[2] ^ s) * columns, columns)
            w_ref[pl.ds(to, columns), :] = ref[pl.ds(at, columns), :]
    return copies


def gate_product(ids, groups, parts):
    columns = groups[0][0].shape[1]
    part_rows, cols = parts[0].shape
    rows = sum(group[0].shape[0] for group in groups)
    blocks, count = len(groups[0]), len(parts)

    def kernel(ids_ref, *refs):
        acc_ref, full_ref, ss_ref, w_ref, sems = refs[-5:]
        copies = lay_rows(ids_ref, refs[-5 - count : -5], full_ref, w_ref, sems, columns)
        start = 0
        for g in range(len(groups)):
            x_refs = refs[g * blocks : (g + 1) * blocks]
            span = x_refs[0].shape[0]
            for r in range(0, span, TILE):
                tile = min(TILE, span - r)
                x = jnp.concatenate([ref[r : r + tile, :] for ref in x_refs], axis=1)
                acc_ref[start + r : start + r + tile, :] = jnp.dot(
                    x, w_ref[...], preferred_element_type=jnp.float32
                )
                total = 0.0
                for ref in x_refs:
                    wide = ref[r : r + tile, :].astype(jnp.float32)
                    total = total + wide * wide
                total = jnp.sum(total, axis=1, keepdims=True)
                ss_ref[start + r : start + r + tile, :] = jnp.broadcast_to(total, (tile, 128))
            start += span
        for copy in copies:
            copy.wait()

    outs = [
        jax.ShapeDtypeStruct((rows, cols), jnp.float32),
        jax.ShapeDtypeStruct((count * part_rows, cols), jnp.bfloat16),
        jax.ShapeDtypeStruct((rows, 128), jnp.float32),
    ]
    operands = [x for group in groups for x in group] + list(parts)
    return local_kernel(
        kernel,
        outs,
        2 * rows * blocks * columns * cols,
        rows * blocks * columns * 2 + rows * cols * 4,
        in_specs=[SMEM] + [VMEM] * len(operands),
        out_specs=[VMEM, HBM, VMEM],
        scratch_shapes=[
            pltpu.VMEM((blocks * columns, cols), jnp.bfloat16),
            pltpu.SemaphoreType.DMA((count,)),
        ],
    )(ids, *operands)


def hidden_product(ids, groups, parts, gate_acc, squares):
    columns = groups[0][0].shape[1]
    part_rows, cols = parts[0].shape
    rows = gate_acc.shape[0]
    blocks, count = len(groups[0]), len(parts)

    def kernel(ids_ref, ga_ref, ss_ref, *refs):
        out_ref, full_ref, w_ref, sems = refs[-4:]
        copies = lay_rows(ids_ref, refs[-4 - count : -4], full_ref, w_ref, sems, columns)
        start = 0
        for g in range(len(groups)):
            x_refs = refs[g * blocks : (g + 1) * blocks]
            span = x_refs[0].shape[0]
            for r in range(0, span, TILE):
                tile = min(TILE, span - r)
                at = slice(start + r, start + r + tile)
                x = jnp.concatenate([ref[r : r + tile, :] for ref in x_refs], axis=1)
                scale = lax.rsqrt(ss_ref[at, 0:1] / (blocks * columns) + epsilon)
                up = jnp.dot(x, w_ref[...], preferred_element_type=jnp.float32) * scale
                gate = ga_ref[at, :] * scale
                out_ref[at, :] = (gate / (1.0 + jnp.exp(-gate)) * up).astype(jnp.bfloat16)
            start += span
        for copy in copies:
            copy.wait()

    outs = [
        jax.ShapeDtypeStruct((rows, cols), jnp.bfloat16),
        jax.ShapeDtypeStruct((count * part_rows, cols), jnp.bfloat16),
    ]
    operands = [x for group in groups for x in group] + list(parts)
    return local_kernel(
        kernel,
        outs,
        2 * rows * blocks * columns * cols,
        rows * blocks * columns * 2 + rows * cols * 4,
        in_specs=[SMEM] + [VMEM] * (2 + len(operands)),
        out_specs=[VMEM, HBM],
        scratch_shapes=[
            pltpu.VMEM((blocks * columns, cols), jnp.bfloat16),
            pltpu.SemaphoreType.DMA((count,)),
        ],
    )(ids, gate_acc, squares, *operands)


def down_product(ids, hidden, parts, full, h, pieces):
    rows, cols = hidden.shape
    count = len(parts)
    piece = parts[0].shape[1]
    full_shape = jax.ShapeDtypeStruct((count, 2, pieces, piece, cols), jnp.bfloat16)

    def kernel(ids_ref, hidden_ref, *refs):
        part_refs = refs[:count]
        sent_ref, kept_ref, full_ref, w_ref, sems = refs[-5:]
        copies = []
        for k, ref in enumerate(part_refs):
            to = full_ref.at[ids_ref[0] ^ k, :, h]
            copies.append(pltpu.make_async_copy(ref, to, sems.at[k]))
            copies[-1].start()
        for k, ref in enumerate(part_refs):
            m = ids_ref[0] ^ ids_ref[1] ^ k
            place, bit = 0, 1
            while bit < count:
                place, bit = 2 * place + (m // bit) % 2, 2 * bit
            for s in range(2):
                w_ref[s, pl.ds(pl.multiple_of(place * piece, piece), piece), :] = ref[
                    ids_ref[2] ^ s
                ]
        for s, ref in ((1, sent_ref), (0, kept_ref)):
            ref[...] = lax.dot_general(
                w_ref[s],
                hidden_ref[...],
                (((1,), (1,)), ((), ())),
                preferred_element_type=jnp.float32,
            ).astype(jnp.bfloat16)
        for copy in copies:
            copy.wait()

    out = jax.ShapeDtypeStruct((count * piece, rows), jnp.bfloat16)
    operands = [ids, hidden, *parts]
    in_specs = [SMEM] + [VMEM] * (1 + count)
    extra = {}
    if full is not None:
        operands.append(full)
        in_specs.append(HBM)
        extra["input_output_aliases"] = {len(operands) - 1: 2}
    return local_kernel(
        kernel,
        [out, out, full_shape],
        4 * count * piece * rows * cols,
        2 * rows * cols + 8 * count * piece * rows,
        in_specs=in_specs,
        out_specs=[VMEM, VMEM, HBM],
        scratch_shapes=[
            pltpu.VMEM((2, count * piece, cols), jnp.bfloat16),
            pltpu.SemaphoreType.DMA((count,)),
        ],
        **extra,
    )(*operands)


def combine(share, backs):
    count = len(backs[0])
    rows = share.shape[1]
    total_cols = sum(back[0].shape[0] for back in backs)

    def kernel(share_ref, *refs):
        parts = []
        for h in range(len(backs)):
            total = 0.0
            for k in range(count):
                term = refs[h * count + k][...].astype(jnp.float32)
                total = total + share_ref[k : k + 1, :] * term
            parts.append(total)
        refs[-1][...] = jnp.concatenate(parts, axis=0).T.astype(jnp.bfloat16)

    flat = [ref for back in backs for ref in back]
    return local_kernel(
        kernel,
        jax.ShapeDtypeStruct((rows, total_cols), jnp.bfloat16),
        2 * rows * total_cols * count,
        2 * rows * total_cols * count,
        in_specs=[VMEM] * (1 + len(flat)),
        out_specs=VMEM,
    )(share, *flat)


PIECES = 4
TILE = 256
RETURNS = ((0, 1, 2), (3,))


def dense_body(tokens, norm_gain, gate_weight, up_weight, down_weight, route, route_weight):
    f32 = jnp.float32
    fs_count, tp_count = lax.axis_size("fs"), lax.axis_size("tp")
    z_count = tp_count // 2
    fs_id, tp_id = lax.axis_index("fs"), lax.axis_index("tp")
    ids = jnp.stack([fs_id, tp_id // 2, tp_id % 2]).astype(jnp.int32)
    tok_rows, _ = tokens.shape
    near = range(fs_count)

    def exchange(parts):
        got = {k: swap(parts[k], "fs", k) for k in far_first(fs_count)}
        got[0] = parts[0]
        return [got[k] for k in near]

    def gather_rows(mine):
        own = {0: mine}
        for m in far_last(z_count):
            top = 1 << (m.bit_length() - 1)
            low = m & -m
            source, distance = (mine, m) if m == low else (own[top], m - top)
            own[m] = swap(source, "tp", 2 * distance)
        sides = [(own[m], swap(own[m], "tp", 1)) for m in range(z_count)]
        return [x for side in sides for x in side]

    fs_tokens = exchange([tokens] * fs_count)
    gate_got = exchange(cast_scaled(ids, gate_weight, norm_gain))
    up_got = exchange(cast_scaled(ids, up_weight, norm_gain))
    down_got = [exchange(parts) for parts in cast_pieces(ids, down_weight, PIECES)]

    groups = [gather_rows(tokens), gather_rows(stack_rows(fs_tokens[1:]))]
    gate_acc, gate_full, squares = gate_product(ids, groups, gate_got)
    hidden, up_full = hidden_product(ids, groups, up_got, gate_acc, squares)

    wanted = fs_id ^ jnp.arange(fs_count, dtype=jnp.int32)
    picks = route.T[None, :, :] == wanted[:, None, None]
    share = jnp.sum(jnp.where(picks, route_weight.T[None, :, :], 0.0), axis=1)

    full, totals = None, []
    for h in range(PIECES):
        sent, kept, full = down_product(ids, hidden, down_got[h], full, h, PIECES)
        came = swap(sent, "tp", 1)
        total = (kept.astype(f32) + came.astype(f32)).astype(jnp.bfloat16)
        step = 1
        while step < z_count:
            half = total.shape[0] // 2
            came = swap(total[half:], "tp", 2 * step)
            total = (total[:half].astype(f32) + came.astype(f32)).astype(jnp.bfloat16)
            step *= 2
        totals.append(total)
    backs = []
    for members in RETURNS:
        total = jnp.concatenate([totals[h] for h in members], axis=0)
        outs = [total[:, k * tok_rows : (k + 1) * tok_rows] for k in near]
        backs.append(exchange(outs))
    mixed = combine(share, backs)

    shape = (1, fs_count * gate_weight.shape[1], gate_weight.shape[2])
    return (mixed, gate_full.reshape(shape), up_full.reshape(shape), full.reshape(shape))


def body(tokens, norm_gain, gate_weight, up_weight, down_weight, route, route_weight):
    fs_count, tp_count = lax.axis_size("fs"), lax.axis_size("tp")
    power = fs_count & (fs_count - 1) == 0
    dense = power and 2 * fs_count == tp_count and fs_count == gate_weight.shape[0] and fs_count <= 4
    run = dense_body if dense else sparse_body
    return run(tokens, norm_gain, gate_weight, up_weight, down_weight, route, route_weight)


def solution(mesh):
    in_specs = (
        P("fs", "tp"),
        P("fs"),
        P(None, "fs", "tp"),
        P(None, "fs", "tp"),
        P(None, "fs", "tp"),
        P("fs", None),
        P("fs", None),
    )
    out_specs = (P("fs", "tp"), P("fs", None, "tp"), P("fs", None, "tp"), P("fs", None, "tp"))
    return jax.shard_map(body, mesh=mesh, in_specs=in_specs, out_specs=out_specs, check_vma=False)
```

```python
import jax
import jax.numpy as jnp
from jax import lax
from jax.experimental import pallas as pl
from jax.experimental.pallas import tpu as pltpu
from jax.sharding import PartitionSpec as P

epsilon = 1e-05


def slot_table(route, block_rows, expert_count):
    pair_ids = route.reshape(-1, block_rows * route.shape[1])
    onehot = (
        pair_ids[:, :, None] == jnp.arange(expert_count, dtype=jnp.int32)[None, None, :]
    ).astype(jnp.int32)
    before = jnp.cumsum(onehot, axis=1) - onehot
    return jnp.sum(before * onehot, axis=2).reshape(route.shape)


def sparse_body(tokens, norm_gain, gate_weight, up_weight, down_weight, route, route_weight):
    experts = gate_weight.shape[0]
    tok_rows = tokens.shape[0]
    columns = tokens.shape[1]
    fs_count = lax.axis_size("fs")
    capacity = 4 * tok_rows // fs_count
    gain_col = norm_gain[None, :, None]
    gate_cast = (gate_weight * gain_col).astype(jnp.bfloat16)
    up_cast = (up_weight * gain_col).astype(jnp.bfloat16)
    down_cast = down_weight.astype(jnp.bfloat16)
    gate_new, up_new, down_new = (
        lax.all_to_all(gate_cast, "fs", split_axis=0, concat_axis=1, tiled=True),
        lax.all_to_all(up_cast, "fs", split_axis=0, concat_axis=1, tiled=True),
        lax.all_to_all(down_cast, "fs", split_axis=0, concat_axis=1, tiled=True),
    )
    slot_of = slot_table(route, tok_rows, experts)
    target = route * capacity + slot_of
    slot_lanes = jnp.arange(experts * capacity, dtype=jnp.int32)
    slot_hits = target[:, :, None] == slot_lanes[None, None, :]
    token_iota = jnp.arange(tok_rows, dtype=jnp.int32)[:, None, None]
    lane_token = jnp.sum(jnp.where(slot_hits, token_iota + 1, 0), axis=(0, 1)) - 1
    lane_token = jnp.where(lane_token < 0, tok_rows, lane_token)
    combine = jnp.sum(jnp.where(slot_hits, route_weight[:, :, None], 0.0), axis=1)
    tok_float = tokens.astype(jnp.float32)
    square_sum = lax.psum(jnp.sum(tok_float * tok_float, axis=1), "tp")
    full_width = columns * lax.axis_size("tp")
    normed = (tok_float * lax.rsqrt(square_sum / full_width + epsilon)[:, None]).astype(
        jnp.bfloat16
    )
    padded = jnp.concatenate([normed, jnp.zeros((1, columns), jnp.bfloat16)], axis=0)
    outgoing = padded[lane_token].reshape(experts, capacity, columns)
    arrived = lax.all_to_all(outgoing, "fs", split_axis=0, concat_axis=0, tiled=True).reshape(
        -1, columns
    )
    piece_rows = lax.all_gather(arrived, "tp", axis=1, tiled=True)
    gate_acc = jnp.dot(piece_rows, gate_new[0], preferred_element_type=jnp.float32)
    up_acc = jnp.dot(piece_rows, up_new[0], preferred_element_type=jnp.float32)
    hidden = (jax.nn.silu(gate_acc) * up_acc).astype(jnp.bfloat16)
    summed = lax.psum_scatter(
        lax.dot_general(
            down_new[0], hidden, (((1,), (1,)), ((), ())), preferred_element_type=jnp.float32
        ).astype(jnp.bfloat16),
        "tp",
        scatter_dimension=0,
        tiled=True,
    )
    own_columns = summed.shape[0]
    outgoing_back = summed.reshape(own_columns, fs_count, capacity)
    returned = lax.all_to_all(outgoing_back, "fs", split_axis=1, concat_axis=1, tiled=True).reshape(
        own_columns, experts * capacity
    )
    mixed = lax.dot_general(
        combine,
        returned.astype(jnp.float32),
        (((1,), (1,)), ((), ())),
        precision=lax.Precision.HIGHEST,
        preferred_element_type=jnp.float32,
    )
    return (mixed.astype(jnp.bfloat16), gate_new, up_new, down_new)


def far_last(count):
    powers = [m for m in range(1, count) if m & (m - 1) == 0]
    return powers[::-1] + [m for m in range(1, count) if m & (m - 1)]


def send_order(count):
    return sorted(range(1, count), key=lambda k: (-bin(k).count("1"), k))


def swap(x, axis, distance):
    count = lax.axis_size(axis)
    return lax.ppermute(x, axis, [(s, s ^ distance) for s in range(count)])


def place_of(m, count):
    place, bit = 0, 1
    while bit < count:
        place, bit = 2 * place + (m // bit) % 2, 2 * bit
    return place


def add(*terms):
    return sum(term.astype(jnp.float32) for term in terms).astype(jnp.bfloat16)


def local_kernel(body, outs, flops=0, moved=0, extra=0, **kwargs):
    def call(*operands):
        held = sum(x.size * x.dtype.itemsize for x in operands)
        held += sum(x.size * x.dtype.itemsize for x in jax.tree.leaves(outs))
        return pl.pallas_call(
            body,
            out_shape=outs,
            cost_estimate=pl.CostEstimate(flops=flops, bytes_accessed=moved, transcendentals=0),
            compiler_params=pltpu.CompilerParams(vmem_limit_bytes=held + extra + GRANT),
            **kwargs,
        )(*operands)

    return call


GRANT = 4 << 20
HBM = pl.BlockSpec(memory_space=pltpu.HBM)
SMEM = pl.BlockSpec(memory_space=pltpu.SMEM)
VMEM = pl.BlockSpec(memory_space=pltpu.VMEM)


def cast_scaled(ids, weight, gain, wanted):
    _, rows, cols = weight.shape
    tile = 128

    def kernel(ids_ref, w_ref, gain_ref, *out_refs):
        for r in range(0, rows, tile):
            column = jnp.broadcast_to(gain_ref[:, r : r + tile], (tile, tile)).T
            column = jnp.concatenate([column] * (cols // tile), axis=1)
            for n, k in enumerate(wanted):
                scaled = w_ref[ids_ref[0] ^ k, r : r + tile] * column
                out_refs[n][r : r + tile, :] = scaled.astype(jnp.bfloat16)

    return local_kernel(
        kernel,
        [jax.ShapeDtypeStruct((rows, cols), jnp.bfloat16)] * len(wanted),
        2 * weight.size,
        6 * weight.size,
        in_specs=[SMEM, VMEM, VMEM],
        out_specs=[VMEM] * len(wanted),
    )(ids, weight, gain[None, :])


def cast_pieces(ids, weight, spans):
    count, rows, cols = weight.shape

    def kernel(ids_ref, w_ref, *out_refs):
        for h, (first, size) in enumerate(spans):
            for k in range(count):
                for side in range(2):
                    start = side * (rows // 2) + first
                    out_refs[h * count + k][side] = w_ref[
                        ids_ref[0] ^ k, start : start + size
                    ].astype(jnp.bfloat16)

    outs = local_kernel(
        kernel,
        [
            jax.ShapeDtypeStruct((2, size, cols), jnp.bfloat16)
            for _, size in spans
            for _ in range(count)
        ],
        2 * weight.size,
        6 * weight.size,
        in_specs=[SMEM, VMEM],
        out_specs=[VMEM] * (count * len(spans)),
    )(ids, weight)
    return [list(outs[h * count : (h + 1) * count]) for h in range(len(spans))]


def stack_rows(parts):
    rows, cols = parts[0].shape

    def kernel(*refs):
        for k in range(len(parts)):
            refs[-1][k * rows : (k + 1) * rows, :] = refs[k][...]

    return local_kernel(
        kernel,
        jax.ShapeDtypeStruct((len(parts) * rows, cols), parts[0].dtype),
        0,
        4 * len(parts) * rows * cols,
        in_specs=[VMEM] * len(parts),
        out_specs=VMEM,
    )(*parts)


def lay_rows(ids_ref, part_refs, full_ref, w_ref, sems, columns):
    part_rows = part_refs[0].shape[0]
    copies = []
    for k, ref in enumerate(part_refs):
        at = pl.multiple_of((ids_ref[0] ^ k) * part_rows, part_rows)
        copies.append(pltpu.make_async_copy(ref, full_ref.at[pl.ds(at, part_rows)], sems.at[k]))
        copies[-1].start()
    for k, ref in enumerate(part_refs):
        m = ids_ref[0] ^ ids_ref[1] ^ k
        for s in range(2):
            to = pl.multiple_of((2 * m + s) * columns, columns)
            at = pl.multiple_of((ids_ref[2] ^ s) * columns, columns)
            w_ref[pl.ds(to, columns), :] = ref[pl.ds(at, columns), :]
    return copies


def gate_product(ids, groups, parts):
    columns = groups[0][0].shape[1]
    part_rows, cols = parts[0].shape
    rows = sum(group[0].shape[0] for group in groups)
    blocks, count = len(groups[0]), len(parts)

    def kernel(ids_ref, *refs):
        acc_ref, full_ref, ss_ref, w_ref, sems = refs[-5:]
        copies = lay_rows(ids_ref, refs[-5 - count : -5], full_ref, w_ref, sems, columns)
        start = 0
        for g in range(len(groups)):
            x_refs = refs[g * blocks : (g + 1) * blocks]
            span = x_refs[0].shape[0]
            for r in range(0, span, TILE):
                tile = min(TILE, span - r)
                x = jnp.concatenate([ref[r : r + tile, :] for ref in x_refs], axis=1)
                acc_ref[start + r : start + r + tile, :] = jnp.dot(
                    x, w_ref[...], preferred_element_type=jnp.float32
                )
                total = 0.0
                for ref in x_refs:
                    wide = ref[r : r + tile, :].astype(jnp.float32)
                    total = total + wide * wide
                total = jnp.sum(total, axis=1, keepdims=True)
                ss_ref[start + r : start + r + tile, :] = jnp.broadcast_to(total, (tile, 128))
            start += span
        for copy in copies:
            copy.wait()

    outs = [
        jax.ShapeDtypeStruct((rows, cols), jnp.float32),
        jax.ShapeDtypeStruct((count * part_rows, cols), jnp.bfloat16),
        jax.ShapeDtypeStruct((rows, 128), jnp.float32),
    ]
    operands = [x for group in groups for x in group] + list(parts)
    return local_kernel(
        kernel,
        outs,
        2 * rows * blocks * columns * cols,
        rows * blocks * columns * 2 + rows * cols * 4,
        in_specs=[SMEM] + [VMEM] * len(operands),
        out_specs=[VMEM, HBM, VMEM],
        scratch_shapes=[
            pltpu.VMEM((blocks * columns, cols), jnp.bfloat16),
            pltpu.SemaphoreType.DMA((count,)),
        ],
    )(ids, *operands)


def hidden_product(ids, groups, parts, gate_acc, squares):
    columns = groups[0][0].shape[1]
    part_rows, cols = parts[0].shape
    rows = gate_acc.shape[0]
    blocks, count = len(groups[0]), len(parts)

    def kernel(ids_ref, ga_ref, ss_ref, *refs):
        out_ref, full_ref, w_ref, sems = refs[-4:]
        copies = lay_rows(ids_ref, refs[-4 - count : -4], full_ref, w_ref, sems, columns)
        start = 0
        for g in range(len(groups)):
            x_refs = refs[g * blocks : (g + 1) * blocks]
            span = x_refs[0].shape[0]
            for r in range(0, span, TILE):
                tile = min(TILE, span - r)
                at = slice(start + r, start + r + tile)
                x = jnp.concatenate([ref[r : r + tile, :] for ref in x_refs], axis=1)
                scale = lax.rsqrt(ss_ref[at, 0:1] / (blocks * columns) + epsilon)
                up = jnp.dot(x, w_ref[...], preferred_element_type=jnp.float32) * scale
                gate = ga_ref[at, :] * scale
                hidden = (gate / (1.0 + jnp.exp(-gate)) * up).astype(jnp.bfloat16)
                out_ref[:, at] = hidden.T
            start += span
        for copy in copies:
            copy.wait()

    outs = [
        jax.ShapeDtypeStruct((cols, rows), jnp.bfloat16),
        jax.ShapeDtypeStruct((count * part_rows, cols), jnp.bfloat16),
    ]
    operands = [x for group in groups for x in group] + list(parts)
    return local_kernel(
        kernel,
        outs,
        2 * rows * blocks * columns * cols,
        rows * blocks * columns * 2 + rows * cols * 4,
        in_specs=[SMEM] + [VMEM] * (2 + len(operands)),
        out_specs=[VMEM, HBM],
        scratch_shapes=[
            pltpu.VMEM((blocks * columns, cols), jnp.bfloat16),
            pltpu.SemaphoreType.DMA((count,)),
        ],
    )(ids, gate_acc, squares, *operands)


def down_product(ids, hidden, parts):
    cols, rows = hidden.shape
    count = len(parts)
    piece = parts[0].shape[1]

    def kernel(ids_ref, hidden_ref, *refs):
        part_refs = refs[:count]
        sent_ref, kept_ref, w_ref = refs[-3:]
        for k, ref in enumerate(part_refs):
            place = place_of(ids_ref[0] ^ ids_ref[1] ^ k, count)
            for s in range(2):
                w_ref[s, pl.ds(pl.multiple_of(place * piece, piece), piece), :] = ref[
                    ids_ref[2] ^ s
                ]
        for s, ref in ((1, sent_ref), (0, kept_ref)):
            ref[...] = jnp.dot(
                w_ref[s], hidden_ref[...], preferred_element_type=jnp.float32
            ).astype(jnp.bfloat16)

    out = jax.ShapeDtypeStruct((count * piece, rows), jnp.bfloat16)
    return local_kernel(
        kernel,
        [out, out],
        4 * count * piece * rows * cols,
        2 * rows * cols + 8 * count * piece * rows,
        in_specs=[SMEM] + [VMEM] * (1 + count),
        out_specs=[VMEM] * 2,
        scratch_shapes=[pltpu.VMEM((2, count * piece, cols), jnp.bfloat16)],
    )(ids, hidden, *parts)


def lay_pieces(ids, pieces):
    count = len(pieces[0])
    cols = pieces[0][0].shape[2]
    sizes = [parts[0].shape[1] for parts in pieces]

    def kernel(ids_ref, *refs):
        full_ref, sems = refs[-2:]
        copies, first = [], 0
        for h, size in enumerate(sizes):
            for k in range(count):
                n = h * count + k
                to = full_ref.at[ids_ref[0] ^ k, :, pl.ds(first, size)]
                copies.append(pltpu.make_async_copy(refs[n], to, sems.at[n]))
                copies[-1].start()
            first += size
        for copy in copies:
            copy.wait()

    flat = [part for parts in pieces for part in parts]
    return local_kernel(
        kernel,
        jax.ShapeDtypeStruct((count, 2, sum(sizes), cols), jnp.bfloat16),
        0,
        8 * count * sum(sizes) * cols,
        in_specs=[SMEM] + [VMEM] * len(flat),
        out_specs=HBM,
        scratch_shapes=[pltpu.SemaphoreType.DMA((len(flat),))],
    )(ids, *flat)


def weighted_cut(kept, came, share):
    cols, rows = kept.shape
    count = share.shape[0]
    cut = rows // count

    def kernel(kept_ref, came_ref, share_ref, *out_refs):
        for k in range(count):
            at = slice(k * cut, (k + 1) * cut)
            total = kept_ref[:, at].astype(jnp.float32) + came_ref[:, at].astype(jnp.float32)
            out_refs[k][...] = (total * share_ref[k : k + 1, :]).astype(jnp.bfloat16)

    return local_kernel(
        kernel,
        [jax.ShapeDtypeStruct((cols, cut), jnp.bfloat16)] * count,
        2 * kept.size,
        6 * kept.size,
        in_specs=[VMEM] * 3,
        out_specs=[VMEM] * count,
    )(kept, came, share)


def combine(share, backs, ready):
    count = len(backs[0])
    rows = share.shape[1]
    total_cols = sum(back[0].shape[0] for back in backs) + sum(terms[0].shape[0] for terms in ready)

    def kernel(share_ref, *refs):
        parts = []
        for h in range(len(backs)):
            total = 0.0
            for k in range(count):
                term = refs[h * count + k][...].astype(jnp.float32)
                total = total + share_ref[k : k + 1, :] * term
            parts.append(total)
        rest = iter(refs[len(flat) : -1])
        for terms in ready:
            parts.append(sum(next(rest)[...].astype(jnp.float32) for _ in terms))
        refs[-1][...] = jnp.concatenate(parts, axis=0).T.astype(jnp.bfloat16)

    flat = [x for back in backs for x in back]
    summed = [x for terms in ready for x in terms]
    return local_kernel(
        kernel,
        jax.ShapeDtypeStruct((rows, total_cols), jnp.bfloat16),
        2 * rows * total_cols * count,
        2 * rows * total_cols * count,
        in_specs=[VMEM] * (1 + len(flat) + len(summed)),
        out_specs=VMEM,
    )(share, *flat, *summed)


SHARES = (4, 3, 5, 4)
PIECES = len(SHARES)
TILE = 256
TP_FIRST = 2


def dense_body(tokens, norm_gain, gate_weight, up_weight, down_weight, route, route_weight):
    fs_count, tp_count = lax.axis_size("fs"), lax.axis_size("tp")
    z_count = tp_count // 2
    fs_id, tp_id = lax.axis_index("fs"), lax.axis_index("tp")
    ids = jnp.stack([fs_id, tp_id // 2, tp_id % 2]).astype(jnp.int32)
    tok_rows, columns = tokens.shape
    near = range(fs_count)
    ends = [columns * sum(SHARES[:h]) // sum(SHARES) for h in range(len(SHARES) + 1)]
    spans = [(a, b - a) for a, b in zip(ends, ends[1:])]

    def exchange(parts):
        got = {k: swap(parts[k], "fs", k) for k in send_order(fs_count)}
        got[0] = parts[0]
        return [got[k] for k in near]

    def gather_rows(mine):
        own = {0: mine}
        for m in far_last(z_count):
            top = 1 << (m.bit_length() - 1)
            low = m & -m
            source, distance = (mine, m) if m == low else (own[top], m - top)
            own[m] = swap(source, "tp", 2 * distance)
        sides = [(own[m], swap(own[m], "tp", 1)) for m in range(z_count)]
        return [x for side in sides for x in side]

    fs_tokens = exchange([tokens] * fs_count)
    gate_got = exchange(cast_scaled(ids, gate_weight, norm_gain, near))
    up_got = exchange(cast_scaled(ids, up_weight, norm_gain, near))
    down_got = [exchange(parts) for parts in cast_pieces(ids, down_weight, spans)]

    groups = [gather_rows(tokens), gather_rows(stack_rows(fs_tokens[1:]))]
    gate_acc, gate_full, squares = gate_product(ids, groups, gate_got)
    hidden, up_full = hidden_product(ids, groups, up_got, gate_acc, squares)

    wanted = fs_id ^ jnp.arange(fs_count, dtype=jnp.int32)
    picks = route.T[None, :, :] == wanted[:, None, None]
    share = jnp.sum(jnp.where(picks, route_weight.T[None, :, :], 0.0), axis=1)

    shares = exchange([share[k : k + 1] for k in near])
    share_all = jnp.concatenate(shares, axis=0)

    def halve(total):
        step = 1
        while step < z_count:
            half = total.shape[0] // 2
            came = swap(total[half:], "tp", 2 * step)
            total = add(total[:half], came)
            step *= 2
        return total

    totals, turned = [], []
    for h in range(PIECES):
        sent, kept = down_product(ids, hidden, down_got[h])
        came = swap(sent, "tp", 1)
        if h < TP_FIRST:
            totals.append(halve(add(kept, came)))
        else:
            cuts = weighted_cut(kept, came, share_all)
            turned.append(add(*exchange(cuts)))
    turned = jnp.concatenate([x.reshape(z_count, -1, tok_rows) for x in turned], axis=1)
    ready = [
        [turned[0]]
        + [swap(turned[place_of(m, z_count)], "tp", 2 * m) for m in range(1, z_count)]
    ]
    total = jnp.concatenate(totals, axis=0)
    outs = [total[:, k * tok_rows : (k + 1) * tok_rows] for k in near]
    full = lay_pieces(ids, down_got)
    mixed = combine(share, [exchange(outs)], ready)

    shape = (1, fs_count * gate_weight.shape[1], gate_weight.shape[2])
    return (mixed, gate_full.reshape(shape), up_full.reshape(shape), full.reshape(shape))


def body(tokens, norm_gain, gate_weight, up_weight, down_weight, route, route_weight):
    fs_count, tp_count = lax.axis_size("fs"), lax.axis_size("tp")
    power = fs_count & (fs_count - 1) == 0
    dense = power and 2 * fs_count == tp_count and fs_count == gate_weight.shape[0] and fs_count <= 4
    run = dense_body if dense else sparse_body
    return run(tokens, norm_gain, gate_weight, up_weight, down_weight, route, route_weight)


def solution(mesh):
    in_specs = (
        P("fs", "tp"),
        P("fs"),
        P(None, "fs", "tp"),
        P(None, "fs", "tp"),
        P(None, "fs", "tp"),
        P("fs", None),
        P("fs", None),
    )
    out_specs = (P("fs", "tp"), P("fs", None, "tp"), P("fs", None, "tp"), P("fs", None, "tp"))
    return jax.shard_map(body, mesh=mesh, in_specs=in_specs, out_specs=out_specs, check_vma=False)
```

```python
import jax
import jax.numpy as jnp
from jax import lax
from jax.experimental import pallas as pl
from jax.experimental.pallas import tpu as pltpu
from jax.sharding import PartitionSpec as P

epsilon = 1e-05


def slot_table(route, block_rows, expert_count):
    pair_ids = route.reshape(-1, block_rows * route.shape[1])
    onehot = (
        pair_ids[:, :, None] == jnp.arange(expert_count, dtype=jnp.int32)[None, None, :]
    ).astype(jnp.int32)
    before = jnp.cumsum(onehot, axis=1) - onehot
    return jnp.sum(before * onehot, axis=2).reshape(route.shape)


def sparse_body(tokens, norm_gain, gate_weight, up_weight, down_weight, route, route_weight):
    experts = gate_weight.shape[0]
    tok_rows = tokens.shape[0]
    columns = tokens.shape[1]
    fs_count = lax.axis_size("fs")
    capacity = 4 * tok_rows // fs_count
    gain_col = norm_gain[None, :, None]
    gate_cast = (gate_weight * gain_col).astype(jnp.bfloat16)
    up_cast = (up_weight * gain_col).astype(jnp.bfloat16)
    down_cast = down_weight.astype(jnp.bfloat16)
    gate_new, up_new, down_new = (
        lax.all_to_all(gate_cast, "fs", split_axis=0, concat_axis=1, tiled=True),
        lax.all_to_all(up_cast, "fs", split_axis=0, concat_axis=1, tiled=True),
        lax.all_to_all(down_cast, "fs", split_axis=0, concat_axis=1, tiled=True),
    )
    slot_of = slot_table(route, tok_rows, experts)
    target = route * capacity + slot_of
    slot_lanes = jnp.arange(experts * capacity, dtype=jnp.int32)
    slot_hits = target[:, :, None] == slot_lanes[None, None, :]
    token_iota = jnp.arange(tok_rows, dtype=jnp.int32)[:, None, None]
    lane_token = jnp.sum(jnp.where(slot_hits, token_iota + 1, 0), axis=(0, 1)) - 1
    lane_token = jnp.where(lane_token < 0, tok_rows, lane_token)
    combine = jnp.sum(jnp.where(slot_hits, route_weight[:, :, None], 0.0), axis=1)
    tok_float = tokens.astype(jnp.float32)
    square_sum = lax.psum(jnp.sum(tok_float * tok_float, axis=1), "tp")
    full_width = columns * lax.axis_size("tp")
    normed = (tok_float * lax.rsqrt(square_sum / full_width + epsilon)[:, None]).astype(
        jnp.bfloat16
    )
    padded = jnp.concatenate([normed, jnp.zeros((1, columns), jnp.bfloat16)], axis=0)
    outgoing = padded[lane_token].reshape(experts, capacity, columns)
    arrived = lax.all_to_all(outgoing, "fs", split_axis=0, concat_axis=0, tiled=True).reshape(
        -1, columns
    )
    piece_rows = lax.all_gather(arrived, "tp", axis=1, tiled=True)
    gate_acc = jnp.dot(piece_rows, gate_new[0], preferred_element_type=jnp.float32)
    up_acc = jnp.dot(piece_rows, up_new[0], preferred_element_type=jnp.float32)
    hidden = (jax.nn.silu(gate_acc) * up_acc).astype(jnp.bfloat16)
    summed = lax.psum_scatter(
        lax.dot_general(
            down_new[0], hidden, (((1,), (1,)), ((), ())), preferred_element_type=jnp.float32
        ).astype(jnp.bfloat16),
        "tp",
        scatter_dimension=0,
        tiled=True,
    )
    own_columns = summed.shape[0]
    outgoing_back = summed.reshape(own_columns, fs_count, capacity)
    returned = lax.all_to_all(outgoing_back, "fs", split_axis=1, concat_axis=1, tiled=True).reshape(
        own_columns, experts * capacity
    )
    mixed = lax.dot_general(
        combine,
        returned.astype(jnp.float32),
        (((1,), (1,)), ((), ())),
        precision=lax.Precision.HIGHEST,
        preferred_element_type=jnp.float32,
    )
    return (mixed.astype(jnp.bfloat16), gate_new, up_new, down_new)


def far_last(count):
    powers = [m for m in range(1, count) if m & (m - 1) == 0]
    return powers[::-1] + [m for m in range(1, count) if m & (m - 1)]


def send_order(count):
    return sorted(range(1, count), key=lambda k: (-bin(k).count("1"), k))


def swap(x, axis, distance):
    count = lax.axis_size(axis)
    return lax.ppermute(x, axis, [(s, s ^ distance) for s in range(count)])


def place_of(m, count):
    place, bit = 0, 1
    while bit < count:
        place, bit = 2 * place + (m // bit) % 2, 2 * bit
    return place


def add(*terms):
    return sum(term.astype(jnp.float32) for term in terms).astype(jnp.bfloat16)


def local_kernel(body, outs, flops=0, moved=0, extra=0, **kwargs):
    def call(*operands):
        held = sum(x.size * x.dtype.itemsize for x in operands)
        held += sum(x.size * x.dtype.itemsize for x in jax.tree.leaves(outs))
        return pl.pallas_call(
            body,
            out_shape=outs,
            cost_estimate=pl.CostEstimate(flops=flops, bytes_accessed=moved, transcendentals=0),
            compiler_params=pltpu.CompilerParams(vmem_limit_bytes=held + extra + GRANT),
            **kwargs,
        )(*operands)

    return call


GRANT = 4 << 20
HBM = pl.BlockSpec(memory_space=pltpu.HBM)
SMEM = pl.BlockSpec(memory_space=pltpu.SMEM)
VMEM = pl.BlockSpec(memory_space=pltpu.VMEM)


def cast_scaled(ids, weight, gain, wanted):
    _, rows, cols = weight.shape
    tile = 128

    def kernel(ids_ref, w_ref, gain_ref, *out_refs):
        for r in range(0, rows, tile):
            column = jnp.broadcast_to(gain_ref[:, r : r + tile], (tile, tile)).T
            column = jnp.concatenate([column] * (cols // tile), axis=1)
            for n, k in enumerate(wanted):
                scaled = w_ref[ids_ref[0] ^ k, r : r + tile] * column
                out_refs[n][r : r + tile, :] = scaled.astype(jnp.bfloat16)

    return local_kernel(
        kernel,
        [jax.ShapeDtypeStruct((rows, cols), jnp.bfloat16)] * len(wanted),
        2 * weight.size,
        6 * weight.size,
        in_specs=[SMEM, VMEM, VMEM],
        out_specs=[VMEM] * len(wanted),
    )(ids, weight, gain[None, :])


def cast_pieces(ids, weight, spans):
    count, rows, cols = weight.shape

    def kernel(ids_ref, w_ref, *out_refs):
        for h, (first, size) in enumerate(spans):
            for k in range(count):
                for side in range(2):
                    start = side * (rows // 2) + first
                    out_refs[h * count + k][side] = w_ref[
                        ids_ref[0] ^ k, start : start + size
                    ].astype(jnp.bfloat16)

    outs = local_kernel(
        kernel,
        [
            jax.ShapeDtypeStruct((2, size, cols), jnp.bfloat16)
            for _, size in spans
            for _ in range(count)
        ],
        2 * weight.size,
        6 * weight.size,
        in_specs=[SMEM, VMEM],
        out_specs=[VMEM] * (count * len(spans)),
    )(ids, weight)
    return [list(outs[h * count : (h + 1) * count]) for h in range(len(spans))]


def stack_rows(parts):
    rows, cols = parts[0].shape

    def kernel(*refs):
        for k in range(len(parts)):
            refs[-1][k * rows : (k + 1) * rows, :] = refs[k][...]

    return local_kernel(
        kernel,
        jax.ShapeDtypeStruct((len(parts) * rows, cols), parts[0].dtype),
        0,
        4 * len(parts) * rows * cols,
        in_specs=[VMEM] * len(parts),
        out_specs=VMEM,
    )(*parts)


def lay_rows(ids_ref, part_refs, full_ref, w_ref, sems, columns):
    part_rows = part_refs[0].shape[0]
    copies = []
    for k, ref in enumerate(part_refs):
        at = pl.multiple_of((ids_ref[0] ^ k) * part_rows, part_rows)
        copies.append(pltpu.make_async_copy(ref, full_ref.at[pl.ds(at, part_rows)], sems.at[k]))
        copies[-1].start()
    for k, ref in enumerate(part_refs):
        m = ids_ref[0] ^ ids_ref[1] ^ k
        for s in range(2):
            to = pl.multiple_of((2 * m + s) * columns, columns)
            at = pl.multiple_of((ids_ref[2] ^ s) * columns, columns)
            w_ref[pl.ds(to, columns), :] = ref[pl.ds(at, columns), :]
    return copies


def gate_product(ids, groups, parts):
    columns = groups[0][0].shape[1]
    part_rows, cols = parts[0].shape
    rows = sum(group[0].shape[0] for group in groups)
    blocks, count = len(groups[0]), len(parts)

    def kernel(ids_ref, *refs):
        acc_ref, full_ref, ss_ref, w_ref, sems = refs[-5:]
        copies = lay_rows(ids_ref, refs[-5 - count : -5], full_ref, w_ref, sems, columns)
        start = 0
        for g in range(len(groups)):
            x_refs = refs[g * blocks : (g + 1) * blocks]
            span = x_refs[0].shape[0]
            for r in range(0, span, TILE):
                tile = min(TILE, span - r)
                x = jnp.concatenate([ref[r : r + tile, :] for ref in x_refs], axis=1)
                acc_ref[start + r : start + r + tile, :] = jnp.dot(
                    x, w_ref[...], preferred_element_type=jnp.float32
                )
                total = 0.0
                for ref in x_refs:
                    wide = ref[r : r + tile, :].astype(jnp.float32)
                    total = total + wide * wide
                total = jnp.sum(total, axis=1, keepdims=True)
                ss_ref[start + r : start + r + tile, :] = jnp.broadcast_to(total, (tile, 128))
            start += span
        for copy in copies:
            copy.wait()

    outs = [
        jax.ShapeDtypeStruct((rows, cols), jnp.float32),
        jax.ShapeDtypeStruct((count * part_rows, cols), jnp.bfloat16),
        jax.ShapeDtypeStruct((rows, 128), jnp.float32),
    ]
    operands = [x for group in groups for x in group] + list(parts)
    return local_kernel(
        kernel,
        outs,
        2 * rows * blocks * columns * cols,
        rows * blocks * columns * 2 + rows * cols * 4,
        in_specs=[SMEM] + [VMEM] * len(operands),
        out_specs=[VMEM, HBM, VMEM],
        scratch_shapes=[
            pltpu.VMEM((blocks * columns, cols), jnp.bfloat16),
            pltpu.SemaphoreType.DMA((count,)),
        ],
    )(ids, *operands)


def hidden_product(ids, groups, parts, gate_acc, squares):
    columns = groups[0][0].shape[1]
    part_rows, cols = parts[0].shape
    rows = gate_acc.shape[0]
    blocks, count = len(groups[0]), len(parts)

    def kernel(ids_ref, ga_ref, ss_ref, *refs):
        out_ref, full_ref, w_ref, sems = refs[-4:]
        copies = lay_rows(ids_ref, refs[-4 - count : -4], full_ref, w_ref, sems, columns)
        start = 0
        for g in range(len(groups)):
            x_refs = refs[g * blocks : (g + 1) * blocks]
            span = x_refs[0].shape[0]
            for r in range(0, span, TILE):
                tile = min(TILE, span - r)
                at = slice(start + r, start + r + tile)
                x = jnp.concatenate([ref[r : r + tile, :] for ref in x_refs], axis=1)
                scale = lax.rsqrt(ss_ref[at, 0:1] / (blocks * columns) + epsilon)
                up = jnp.dot(x, w_ref[...], preferred_element_type=jnp.float32) * scale
                gate = ga_ref[at, :] * scale
                hidden = (gate / (1.0 + jnp.exp(-gate)) * up).astype(jnp.bfloat16)
                out_ref[:, at] = hidden.T
            start += span
        for copy in copies:
            copy.wait()

    outs = [
        jax.ShapeDtypeStruct((cols, rows), jnp.bfloat16),
        jax.ShapeDtypeStruct((count * part_rows, cols), jnp.bfloat16),
    ]
    operands = [x for group in groups for x in group] + list(parts)
    return local_kernel(
        kernel,
        outs,
        2 * rows * blocks * columns * cols,
        rows * blocks * columns * 2 + rows * cols * 4,
        in_specs=[SMEM] + [VMEM] * (2 + len(operands)),
        out_specs=[VMEM, HBM],
        scratch_shapes=[
            pltpu.VMEM((blocks * columns, cols), jnp.bfloat16),
            pltpu.SemaphoreType.DMA((count,)),
        ],
    )(ids, gate_acc, squares, *operands)


def down_product(ids, hidden, parts):
    cols, rows = hidden.shape
    count = len(parts)
    piece = parts[0].shape[1]

    def kernel(ids_ref, hidden_ref, *refs):
        part_refs = refs[:count]
        sent_ref, kept_ref, w_ref = refs[-3:]
        for k, ref in enumerate(part_refs):
            place = place_of(ids_ref[0] ^ ids_ref[1] ^ k, count)
            for s in range(2):
                w_ref[s, pl.ds(pl.multiple_of(place * piece, piece), piece), :] = ref[
                    ids_ref[2] ^ s
                ]
        for s, ref in ((1, sent_ref), (0, kept_ref)):
            ref[...] = jnp.dot(
                w_ref[s], hidden_ref[...], preferred_element_type=jnp.float32
            ).astype(jnp.bfloat16)

    out = jax.ShapeDtypeStruct((count * piece, rows), jnp.bfloat16)
    return local_kernel(
        kernel,
        [out, out],
        4 * count * piece * rows * cols,
        2 * rows * cols + 8 * count * piece * rows,
        in_specs=[SMEM] + [VMEM] * (1 + count),
        out_specs=[VMEM] * 2,
        scratch_shapes=[pltpu.VMEM((2, count * piece, cols), jnp.bfloat16)],
    )(ids, hidden, *parts)


def lay_pieces(ids, pieces):
    count = len(pieces[0])
    cols = pieces[0][0].shape[2]
    sizes = [parts[0].shape[1] for parts in pieces]

    def kernel(ids_ref, *refs):
        full_ref, sems = refs[-2:]
        copies, first = [], 0
        for h, size in enumerate(sizes):
            for k in range(count):
                n = h * count + k
                to = full_ref.at[ids_ref[0] ^ k, :, pl.ds(first, size)]
                copies.append(pltpu.make_async_copy(refs[n], to, sems.at[n]))
                copies[-1].start()
            first += size
        for copy in copies:
            copy.wait()

    flat = [part for parts in pieces for part in parts]
    return local_kernel(
        kernel,
        jax.ShapeDtypeStruct((count, 2, sum(sizes), cols), jnp.bfloat16),
        0,
        8 * count * sum(sizes) * cols,
        in_specs=[SMEM] + [VMEM] * len(flat),
        out_specs=HBM,
        scratch_shapes=[pltpu.SemaphoreType.DMA((len(flat),))],
    )(ids, *flat)


def weighted_cut(kept, came, share):
    cols, rows = kept.shape
    count = share.shape[0]
    cut = rows // count

    def kernel(kept_ref, came_ref, share_ref, *out_refs):
        for k in range(count):
            at = slice(k * cut, (k + 1) * cut)
            total = kept_ref[:, at].astype(jnp.float32) + came_ref[:, at].astype(jnp.float32)
            out_refs[k][...] = (total * share_ref[k : k + 1, :]).astype(jnp.bfloat16)

    return local_kernel(
        kernel,
        [jax.ShapeDtypeStruct((cols, cut), jnp.bfloat16)] * count,
        2 * kept.size,
        6 * kept.size,
        in_specs=[VMEM] * 3,
        out_specs=[VMEM] * count,
    )(kept, came, share)


def weighted_halves(pairs, share):
    count, cut = share.shape
    cols = sum(pair[0].shape[0] for pair in pairs)
    groups = sorted(range(count), key=lambda k: place_of(k, count))

    def kernel(share_ref, *refs):
        kept_ref, sent_ref = refs[-2:]
        first = 0
        for one, two in zip(refs[:-2:2], refs[1:-2:2]):
            at = slice(first, first + one.shape[0])
            for n, k in enumerate(groups):
                span = slice(k * cut, (k + 1) * cut)
                total = one[:, span].astype(jnp.float32) + two[:, span].astype(jnp.float32)
                ref, place = (kept_ref, n) if 2 * n < count else (sent_ref, n - count // 2)
                value = (total * share_ref[k : k + 1, :]).astype(jnp.bfloat16)
                ref[at, place * cut : (place + 1) * cut] = value
            first += one.shape[0]

    flat = [x for pair in pairs for x in pair]
    return local_kernel(
        kernel,
        [jax.ShapeDtypeStruct((cols, count // 2 * cut), jnp.bfloat16)] * 2,
        2 * cols * count * cut,
        6 * cols * count * cut,
        in_specs=[VMEM] * (1 + len(flat)),
        out_specs=[VMEM] * 2,
    )(share, *flat)


def combine(ready):
    rows = ready[0][0].shape[1]
    total_cols = sum(terms[0].shape[0] for terms in ready)

    def kernel(*refs):
        parts = []
        rest = iter(refs[:-1])
        for terms in ready:
            parts.append(sum(next(rest)[...].astype(jnp.float32) for _ in terms))
        refs[-1][...] = jnp.concatenate(parts, axis=0).T.astype(jnp.bfloat16)

    summed = [x for terms in ready for x in terms]
    return local_kernel(
        kernel,
        jax.ShapeDtypeStruct((rows, total_cols), jnp.bfloat16),
        2 * rows * total_cols * len(summed),
        2 * rows * total_cols * len(summed),
        in_specs=[VMEM] * len(summed),
        out_specs=VMEM,
    )(*summed)


SHARES = (4, 4, 4, 4)
PIECES = len(SHARES)
TILE = 256
TP_FIRST = 2


def dense_body(tokens, norm_gain, gate_weight, up_weight, down_weight, route, route_weight):
    fs_count, tp_count = lax.axis_size("fs"), lax.axis_size("tp")
    z_count = tp_count // 2
    fs_id, tp_id = lax.axis_index("fs"), lax.axis_index("tp")
    ids = jnp.stack([fs_id, tp_id // 2, tp_id % 2]).astype(jnp.int32)
    tok_rows, columns = tokens.shape
    near = range(fs_count)
    ends = [columns * sum(SHARES[:h]) // sum(SHARES) for h in range(len(SHARES) + 1)]
    spans = [(a, b - a) for a, b in zip(ends, ends[1:])]

    def exchange(parts):
        got = {k: swap(parts[k], "fs", k) for k in send_order(fs_count)}
        got[0] = parts[0]
        return [got[k] for k in near]

    def gather_rows(mine):
        own = {0: mine}
        for m in far_last(z_count):
            top = 1 << (m.bit_length() - 1)
            low = m & -m
            source, distance = (mine, m) if m == low else (own[top], m - top)
            own[m] = swap(source, "tp", 2 * distance)
        sides = [(own[m], swap(own[m], "tp", 1)) for m in range(z_count)]
        return [x for side in sides for x in side]

    fs_tokens = exchange([tokens] * fs_count)
    gate_got = exchange(cast_scaled(ids, gate_weight, norm_gain, near))
    up_got = exchange(cast_scaled(ids, up_weight, norm_gain, near))
    down_got = [exchange(parts) for parts in cast_pieces(ids, down_weight, spans)]

    groups = [gather_rows(tokens), gather_rows(stack_rows(fs_tokens[1:]))]
    gate_acc, gate_full, squares = gate_product(ids, groups, gate_got)
    hidden, up_full = hidden_product(ids, groups, up_got, gate_acc, squares)

    wanted = fs_id ^ jnp.arange(fs_count, dtype=jnp.int32)
    picks = route.T[None, :, :] == wanted[:, None, None]
    share = jnp.sum(jnp.where(picks, route_weight.T[None, :, :], 0.0), axis=1)

    shares = exchange([share[k : k + 1] for k in near])
    share_all = jnp.concatenate(shares, axis=0)

    def halve(total):
        step, came = 1, None
        while step < z_count:
            if came is not None:
                total = add(total, came)
            half = total.shape[0] // 2
            came = swap(total[half:], "tp", 2 * step)
            total, step = total[:half], 2 * step
        return total, came

    totals, turned = [], []
    for h in range(PIECES):
        sent, kept = down_product(ids, hidden, down_got[h])
        came = swap(sent, "tp", 1)
        if h < TP_FIRST:
            totals.append(halve(add(kept, came)))
        else:
            cuts = weighted_cut(kept, came, share_all)
            turned.append(add(*exchange(cuts)))
    turned = jnp.concatenate([x.reshape(z_count, -1, tok_rows) for x in turned], axis=1)
    last = [turned[0]]
    last += [swap(turned[place_of(m, z_count)], "tp", 2 * m) for m in range(1, z_count)]
    total, sent = weighted_halves(totals, share_all)
    came, step = swap(sent, "fs", 1), 2
    while step < fs_count:
        total = add(total, came)
        half = total.shape[1] // 2
        came = swap(total[:, half:], "fs", step)
        total, step = total[:, :half], 2 * step
    full = lay_pieces(ids, down_got)
    mixed = combine([[total, came], last])

    shape = (1, fs_count * gate_weight.shape[1], gate_weight.shape[2])
    return (mixed, gate_full.reshape(shape), up_full.reshape(shape), full.reshape(shape))


def body(tokens, norm_gain, gate_weight, up_weight, down_weight, route, route_weight):
    fs_count, tp_count = lax.axis_size("fs"), lax.axis_size("tp")
    power = fs_count & (fs_count - 1) == 0
    dense = power and 2 * fs_count == tp_count and fs_count == gate_weight.shape[0] and fs_count <= 4
    run = dense_body if dense else sparse_body
    return run(tokens, norm_gain, gate_weight, up_weight, down_weight, route, route_weight)


def solution(mesh):
    in_specs = (
        P("fs", "tp"),
        P("fs"),
        P(None, "fs", "tp"),
        P(None, "fs", "tp"),
        P(None, "fs", "tp"),
        P("fs", None),
        P("fs", None),
    )
    out_specs = (P("fs", "tp"), P("fs", None, "tp"), P("fs", None, "tp"), P("fs", None, "tp"))
    return jax.shard_map(body, mesh=mesh, in_specs=in_specs, out_specs=out_specs, check_vma=False)
```
